256 devices in a mesh: grp: 2 (over z), ep: 16 (over y, core), tp: 8 (over x).
Axes of the slice: x: 8, y: 8, z: 2, core: 2. Of those that a mesh axis runs over, the one named last changes fastest.
The devices are a block of a 8x8x16 slice.
Arguments:
- tokens: bfloat16 [8192, 4096], P(('grp', 'ep')), parts along dimension 0, may hold values from -6 to 6
- expert_ids: int32 [8192, 2], P(('grp', 'ep')), parts along dimension 0, may hold values from 0 to 15, as said below
- gates: float32 [8192, 2], P(('grp', 'ep')), parts along dimension 0, may hold values from 0.1 to 1
- w_gate: bfloat16 [16, 4096, 2048], P('ep', None, 'tp'), may hold values from -0.09375 to 0.09375
- w_up: bfloat16 [16, 4096, 2048], P('ep', None, 'tp'), may hold values from -0.09375 to 0.09375
- w_down: bfloat16 [16, 2048, 4096], P('ep', 'tp'), may hold values from -0.79549513 to 0.79549513, as said below
- norm_gain: float32 [4096], P('tp'), may hold values from 0.1 to 1.9
- norm_bias: float32 [4096], P('tp'), may hold values from -1.5 to 1.5
Outputs:
- normed: bfloat16 [8192, 4096], P(('grp', 'ep'), 'tp'), parts along dimension 0
The draws below stay inside these ranges and needn't reach their ends.
There are 2 independent parts, one for each index of `grp`. The reference program is written for one: setup_inputs(seed, part) draws one part's arguments, and reference() takes and returns one part's arrays. A program takes and returns all parts, laid end to end along the dimension named above; an argument that names none is the same for every part. Nothing has to cross between parts.
Inputs may be any that keep to these rules, and one draw needn't show every extreme that they name: `expert_ids`: each row names 2 different experts, both in the same group of 4 consecutive expert numbers. Within one aligned block of 256 rows no expert is named more than 64 times, and in every draw some expert is named exactly 64 times in every block. `w_down`: down projection weights.
All inputs are finite; a program needn't handle non-finite values.
Results may differ from the reference program's by a relative error of at most 0.014.
Values may be sent and summed in bfloat16 or wider, within the bound.
No kernel may reach another device: no remote copies, remote signals or barrier semaphores. Data moves between devices by JAX's collectives and lax.ppermute only.
A program may use at most 128 MiB of HBM per device.

```python
import math
import jax
import jax.numpy as jnp
from jax import lax

D = 4096
FF = 2048
GROUPS = 4
EXPERTS_PER_GROUP = 4
TOPK = 2
TOK_DEV = 256
EXPERTS = 16
CAP = 64
SLOTS = 1024
FF_DEV = 256
TOKENS = 4096
N_EP = 16
N_TP = 8


def route_block(block_key, busy_group):
    key_weights, key_labels, key_shuffle = jax.random.split(block_key, 3)
    weights = jax.random.randint(key_weights, (GROUPS,), 4, 9)
    is_busy = jnp.arange(GROUPS) == busy_group
    weights = jnp.where(is_busy, 0, weights)
    busy_count = TOK_DEV // 2
    remainder = TOK_DEV - busy_count
    counts = remainder * weights // jnp.sum(weights)
    leftover = remainder - jnp.sum(counts)
    first_other = jnp.argmin(is_busy.astype(jnp.int32))
    counts = counts + leftover * (jnp.arange(GROUPS) == first_other).astype(jnp.int32)
    counts = jnp.where(is_busy, busy_count, counts)
    group_ends = jnp.cumsum(counts)
    group_starts = group_ends - counts
    position = jnp.arange(TOK_DEV)
    group_of = jnp.sum((position[:, None] >= group_ends[None, :]).astype(jnp.int32), axis=1)
    within = position - group_starts[group_of]
    first_table = jnp.array([0, 2, 0, 1, 0, 1], jnp.int32)
    second_table = jnp.array([1, 3, 2, 3, 3, 2], jnp.int32)
    relabel = jax.vmap(lambda label_key: jax.random.permutation(label_key, EXPERTS_PER_GROUP))(jax.random.split(key_labels, GROUPS))
    group_base = group_of * EXPERTS_PER_GROUP
    first_expert = group_base + relabel[group_of, first_table[within % 6]]
    second_expert = group_base + relabel[group_of, second_table[within % 6]]
    chosen = jnp.stack([first_expert, second_expert], axis=1).astype(jnp.int32)
    shuffle = jax.random.permutation(key_shuffle, TOK_DEV)
    return chosen[shuffle]


def draw_expert_ids(key, part):
    busy_group = jax.random.randint(jax.random.fold_in(key, 7), (), 0, GROUPS)
    block_keys = jax.random.split(jax.random.fold_in(key, 11), TOKENS // TOK_DEV)
    chosen = jax.vmap(route_block, in_axes=(0, None))(block_keys, busy_group)
    return chosen.reshape(TOKENS, TOPK).astype(jnp.int32)


def draw_w_down(key, part):
    noise = jnp.clip(jax.random.normal(jax.random.fold_in(key, 3), (EXPERTS, FF, D), jnp.float32), -6.0, 6.0)
    columns = 0.6 * jnp.exp(math.log(3.0) * jnp.arange(D, dtype=jnp.float32) / (D - 1))
    return (noise * FF ** (-0.5) * columns).astype(jnp.bfloat16)


def shard_levels(key, extent, shards, low, top_value):
    gain = 1.0
    for dim, shards_of in shards:
        draws = jax.random.uniform(jax.random.fold_in(jax.random.fold_in(key, 6), dim), (shards_of,), jnp.float32, low / len(shards), top_value / len(shards))
        gain = gain * jnp.repeat(jnp.exp(draws), extent[dim] // shards_of).reshape((-1,) + (1,) * (len(extent) - 1 - dim))
    return gain


def normal_values(key, shape, width, limit, cuts=(), kind=jnp.bfloat16):
    drawn = width * jax.random.normal(key, shape, jnp.float32)
    if cuts:
        drawn = drawn * shard_levels(key, shape, cuts, -0.22, 0.18)
    return jnp.clip(drawn, -limit, limit).astype(kind)


def setup_inputs(seed: int = 0, part: int = 0) -> dict:
    seeds = jax.random.split(jax.random.key(seed), 9)
    part_splits = jax.random.split(jax.random.fold_in(seeds[8], part), 9)
    tokens = normal_values(part_splits[0], (TOKENS, D), 1.0, 6.0, ((0, 16),))
    expert_ids = draw_expert_ids(jax.random.fold_in(jax.random.fold_in(seeds[8], part), 71), part)
    gates = jnp.clip(0.1 + 0.9 * jax.random.uniform(part_splits[2], (TOKENS, TOPK), jnp.float32) ** shard_levels(part_splits[2], (TOKENS, TOPK), ((0, 16),), -0.2, 0.2), 0.1, 1.0)
    w_gate = normal_values(seeds[3], (EXPERTS, D, FF), D ** -0.5, 0.09375, ((0, 16), (2, 8)))
    w_up = normal_values(seeds[4], (EXPERTS, D, FF), D ** -0.5, 0.09375, ((0, 16), (2, 8)))
    w_down = draw_w_down(jax.random.fold_in(seeds[8], 71), part)
    norm_gain = jnp.clip(1.0 + 0.18 * jax.random.normal(seeds[6], (D,), jnp.float32), 0.1, 1.9)
    norm_bias = normal_values(seeds[7], (D,), 0.3, 1.5, ((0, 8),), jnp.float32)
    return dict(tokens=tokens, expert_ids=expert_ids, gates=gates, w_gate=w_gate, w_up=w_up, w_down=w_down, norm_gain=norm_gain, norm_bias=norm_bias)


norm_eps = 1e-05

def run_expert(operands):
    routed, gate_w, up_w, down_w = operands
    gate_part = jnp.dot(routed, gate_w, preferred_element_type=jnp.float32)
    up_part = jnp.dot(routed, up_w, preferred_element_type=jnp.float32)
    hidden = (jax.nn.silu(gate_part) * up_part).astype(jnp.bfloat16)
    blocks = hidden.reshape(SLOTS, N_TP, FF_DEV).astype(jnp.float32)
    down_blocks = down_w.reshape(N_TP, FF_DEV, D).astype(jnp.float32)
    partial_value = jnp.einsum('rjf,jfd->jrd', blocks, down_blocks).astype(jnp.bfloat16)
    partial_value = lax.optimization_barrier(partial_value)
    return lax.optimization_barrier(jnp.sum(partial_value.astype(jnp.float32), axis=0)).astype(jnp.bfloat16)

def reference(tokens, expert_ids, gates, w_gate, w_up, w_down, norm_gain, norm_bias):
    flat_ids = expert_ids.reshape(N_EP, TOK_DEV * TOPK)
    onehot = (flat_ids[:, :, None] == jnp.arange(EXPERTS, dtype=jnp.int32)[None, None, :]).astype(jnp.int32)
    position = lax.optimization_barrier(jnp.sum((jnp.cumsum(onehot, axis=1) - 1) * onehot, axis=2))
    source_block = jnp.arange(N_EP, dtype=jnp.int32)[:, None]
    target = (flat_ids * SLOTS + source_block * CAP + position).reshape(-1).astype(jnp.int32)
    token_of = jnp.arange(TOKENS * TOPK, dtype=jnp.int32) // TOPK
    source = jnp.zeros((EXPERTS * SLOTS,), jnp.int32).at[target].set(token_of)
    filled = jnp.zeros((EXPERTS * SLOTS,), jnp.bool_).at[target].set(True)
    routed = jnp.where(filled[:, None], tokens[source], jnp.zeros((), jnp.bfloat16)).reshape(EXPERTS, SLOTS, D)
    expert_out = lax.map(run_expert, (routed, w_gate, w_up, w_down))
    picked = expert_out.reshape(EXPERTS * SLOTS, D)[target].reshape(TOKENS, TOPK, D)
    combined = lax.optimization_barrier(jnp.sum(picked.astype(jnp.float32) * gates[:, :, None], axis=1))
    row_mean = lax.optimization_barrier(jnp.mean(combined, axis=1, keepdims=True))
    centred = combined - row_mean
    row_var = lax.optimization_barrier(jnp.mean(centred * centred, axis=1, keepdims=True))
    normed = centred * lax.rsqrt(row_var + norm_eps) * norm_gain + norm_bias
    return normed.astype(jnp.bfloat16)
```

```python
import jax
import jax.numpy as jnp
from jax import lax
from jax.sharding import PartitionSpec as P

D = 4096
EXPERTS = 16
CAP = 64
RING_PARTS = 3
ALL_PARTS = 4

norm_eps = 1e-05


def f32_dot(a, b, dims=(((1,), (0,)), ((), ()))):
    return lax.dot_general(a, b, dims, preferred_element_type=jnp.float32)


def route(expert_ids, gates):
    ids = expert_ids.T
    tok = ids.shape[1]
    experts = jnp.arange(EXPERTS, dtype=jnp.int32)[:, None]
    first = ids[0][None, :] == experts
    second = ids[1][None, :] == experts
    named = jnp.logical_or(first, second).astype(jnp.bfloat16)
    row = jnp.arange(tok, dtype=jnp.int32)
    before = (row[:, None] < row[None, :]).astype(jnp.bfloat16)
    slot = f32_dot(named, before).astype(jnp.int32) + experts * CAP
    target0 = jnp.sum(jnp.where(first, slot, 0), axis=0)
    target1 = jnp.sum(jnp.where(second, slot, 0), axis=0)
    slots = jnp.arange(EXPERTS * CAP, dtype=jnp.int32)[:, None]
    at0 = slots == target0[None, :]
    at1 = slots == target1[None, :]
    send = jnp.logical_or(at0, at1).astype(jnp.bfloat16)
    g = gates.T
    weight = jnp.where(at0, g[0][None, :], 0.0) + jnp.where(at1, g[1][None, :], 0.0)
    high = lax.reduce_precision(weight, 8, 7)
    return send, high.astype(jnp.bfloat16), (weight - high).astype(jnp.bfloat16)


def on_device(tokens, expert_ids, gates, w_gate, w_up, w_down, norm_gain, norm_bias):
    tok_rows, width = tokens.shape
    n_tp = lax.axis_size("tp")
    n_ep = lax.axis_size("ep")
    me = lax.axis_index("tp")
    piece = norm_gain.shape[0]
    ring_piece = piece * RING_PARTS // ALL_PARTS
    flat_piece = piece - ring_piece
    ring_width = ring_piece * n_tp
    flat_width = flat_piece * n_tp
    right = [(i, (i + 1) % n_tp) for i in range(n_tp)]
    left = [(i, (i - 1) % n_tp) for i in range(n_tp)]
    far = n_tp // 2

    def at(i):
        return lax.rem(me + i + n_tp, n_tp)

    send, weight_high, weight_low = route(expert_ids, gates)
    own = lax.dynamic_slice_in_dim(tokens, me * ring_piece, ring_piece, 1)
    out1 = f32_dot(send, own).astype(jnp.bfloat16).reshape(n_ep, CAP, ring_piece)
    out2 = f32_dot(send, tokens[:, ring_width:]).astype(jnp.bfloat16).reshape(n_ep, CAP, flat_width)
    got1 = lax.all_to_all(out1, "ep", 0, 0, tiled=True).reshape(n_ep * CAP, ring_piece)
    got1, out2 = lax.optimization_barrier((got1, out2))
    got2 = lax.all_to_all(out2, "ep", 0, 0, tiled=True).reshape(n_ep * CAP, flat_width)

    wg = w_gate[0]
    wu = w_up[0]
    wd = w_down[0]
    rows = n_ep * CAP
    half = rows // 2

    def gate_up(x, start, size):
        g = f32_dot(x, lax.dynamic_slice_in_dim(wg, start, size, 0))
        u = f32_dot(x, lax.dynamic_slice_in_dim(wu, start, size, 0))
        return g, u

    hops = ((far, n_tp - 1 - far), (n_tp - 1 - far, far))
    cur = []
    acc = []
    for h in range(2):
        x = got1[h * half : (h + 1) * half]
        cur.append([x, x])
        acc.append(gate_up(x, me * ring_piece, ring_piece))
    for s in range(1, far + 1):
        for h in range(2):
            for d, perm in enumerate((right, left)):
                if s <= hops[h][d]:
                    cur[h][d] = lax.ppermute(cur[h][d], "tp", perm)
                    origin = at(-s) if d == 0 else at(s)
                    g, u = gate_up(cur[h][d], origin * ring_piece, ring_piece)
                    acc[h] = (acc[h][0] + g, acc[h][1] + u)
    hidden = []
    for h in range(2):
        g, u = gate_up(got2[h * half : (h + 1) * half], ring_width, flat_width)
        g = acc[h][0] + g
        u = acc[h][1] + u
        hidden.append((g / (1.0 + jnp.exp(-g)) * u).astype(jnp.bfloat16))

    wd2 = wd.reshape(wd.shape[0], n_tp, piece)[:, :, ring_piece:].reshape(wd.shape[0], flat_width)
    back2 = jnp.concatenate([f32_dot(x, wd2).astype(jnp.bfloat16) for x in hidden], axis=0)
    home2 = lax.all_to_all(back2.reshape(n_ep, CAP, flat_width), "ep", 0, 0, tiled=True).reshape(rows, flat_width)

    def down(h, target):
        cols = lax.dynamic_slice_in_dim(wd, target * piece, ring_piece, 1)
        return f32_dot(hidden[h], cols)

    moving = [[None, None], [None, None]]
    for s in range(far, 0, -1):
        for h in range(2):
            for d, perm in enumerate((right, left)):
                if s <= hops[h][d]:
                    target = at(s) if d == 0 else at(-s)
                    part = down(h, target)
                    if moving[h][d] is not None:
                        part = part + moving[h][d].astype(jnp.float32)
                    moving[h][d] = lax.ppermute(part.astype(jnp.bfloat16), "tp", perm)
    back1 = []
    for h in range(2):
        total = down(h, me) + moving[h][0].astype(jnp.float32) + moving[h][1].astype(jnp.float32)
        back1.append(total.astype(jnp.bfloat16))
    back1 = jnp.concatenate(back1, axis=0).reshape(n_ep, CAP, ring_piece)
    home1 = lax.all_to_all(back1, "ep", 0, 0, tiled=True).reshape(rows, ring_piece)

    first_dims = (((0,), (0,)), ((), ()))

    def combine(x):
        return f32_dot(weight_high, x, first_dims) + f32_dot(weight_low, x, first_dims)

    mixed2 = combine(home2).astype(jnp.bfloat16).reshape(tok_rows, n_tp, flat_piece)
    mixed2 = lax.all_to_all(mixed2.transpose(1, 0, 2), "tp", 0, 0, tiled=True)
    mixed2 = jnp.sum(mixed2.astype(jnp.float32), axis=0)
    combined = jnp.concatenate([combine(home1), mixed2], axis=1)

    stats = jnp.stack([jnp.sum(combined, axis=1), jnp.sum(combined * combined, axis=1)])
    stats = lax.all_to_all(jnp.broadcast_to(stats[None], (n_tp, *stats.shape)), "tp", 0, 0, tiled=True)
    stats = jnp.sum(stats, axis=0)
    row_mean = stats[0] / D
    row_var = stats[1] / D - row_mean * row_mean
    normed = (combined - row_mean[:, None]) * lax.rsqrt(
        row_var[:, None] + norm_eps
    ) * norm_gain + norm_bias
    return normed.astype(jnp.bfloat16)


def solution(mesh):
    return jax.shard_map(
        on_device,
        mesh=mesh,
        in_specs=(
            P(("grp", "ep"), None),
            P(("grp", "ep"), None),
            P(("grp", "ep"), None),
            P("ep", None, "tp"),
            P("ep", None, "tp"),
            P("ep", "tp", None),
            P("tp"),
            P("tp"),
        ),
        out_specs=P(("grp", "ep"), "tp"),
        check_vma=False,
    )
```

```python
import jax
import jax.numpy as jnp
from jax import lax
from jax.sharding import PartitionSpec as P

D = 4096
EXPERTS = 16
CAP = 64
RING_PARTS = 3
ALL_PARTS = 4

norm_eps = 1e-05


def f32_dot(a, b, dims=(((1,), (0,)), ((), ()))):
    return lax.dot_general(a, b, dims, preferred_element_type=jnp.float32)


def route(expert_ids, gates):
    ids = expert_ids.T
    tok = ids.shape[1]
    experts = jnp.arange(EXPERTS, dtype=jnp.int32)[:, None]
    first = ids[0][None, :] == experts
    second = ids[1][None, :] == experts
    named = jnp.logical_or(first, second).astype(jnp.bfloat16)
    row = jnp.arange(tok, dtype=jnp.int32)
    before = (row[:, None] < row[None, :]).astype(jnp.bfloat16)
    slot = f32_dot(named, before).astype(jnp.int32) + experts * CAP
    target0 = jnp.sum(jnp.where(first, slot, 0), axis=0)
    target1 = jnp.sum(jnp.where(second, slot, 0), axis=0)
    slots = jnp.arange(EXPERTS * CAP, dtype=jnp.int32)[:, None]
    at0 = slots == target0[None, :]
    at1 = slots == target1[None, :]
    send = jnp.logical_or(at0, at1).astype(jnp.bfloat16)
    g = gates.T
    weight = jnp.where(at0, g[0][None, :], 0.0) + jnp.where(at1, g[1][None, :], 0.0)
    high = lax.reduce_precision(weight, 8, 7)
    return send, high.astype(jnp.bfloat16), (weight - high).astype(jnp.bfloat16)


def layer(tokens, expert_ids, gates, w_gate, w_up, w_down, norm_gain, norm_bias):
    n_tp = lax.axis_size("tp")
    n_ep = lax.axis_size("ep")
    me = lax.axis_index("tp")
    piece = norm_gain.shape[0]
    ring_piece = piece * RING_PARTS // ALL_PARTS
    flat_piece = piece - ring_piece
    ring_width = ring_piece * n_tp
    flat_width = flat_piece * n_tp
    right = [(i, (i + 1) % n_tp) for i in range(n_tp)]
    left = [(i, (i - 1) % n_tp) for i in range(n_tp)]
    far = n_tp // 2

    def at(i):
        return lax.rem(me + i + n_tp, n_tp)

    send, weight_high, weight_low = route(expert_ids, gates)
    own = lax.dynamic_slice_in_dim(tokens, me * ring_piece, ring_piece, 1)
    out1 = f32_dot(send, own).astype(jnp.bfloat16).reshape(n_ep, CAP, ring_piece)
    out2 = f32_dot(send, tokens[:, ring_width:]).astype(jnp.bfloat16).reshape(n_ep, CAP, flat_width)
    got1 = lax.all_to_all(out1, "ep", 0, 0, tiled=True).reshape(n_ep * CAP, ring_piece)
    w_both = lax.optimization_barrier(jnp.concatenate([w_gate[0], w_up[0]], axis=1))
    hidden_width = w_up.shape[2]
    got1, out2 = lax.optimization_barrier((got1, out2))
    got2 = lax.all_to_all(out2, "ep", 0, 0, tiled=True).reshape(n_ep * CAP, flat_width)

    wd = w_down[0]
    rows = n_ep * CAP
    half = rows // 2

    def gate_up(x, start, size):
        return f32_dot(x, lax.dynamic_slice_in_dim(w_both, start, size, 0))

    hops = ((far, n_tp - 1 - far), (n_tp - 1 - far, far))
    cur = []
    acc = []
    for h in range(2):
        x = got1[h * half : (h + 1) * half]
        cur.append([x, x])
        acc.append(None)
    for s in range(1, far + 1):
        for h in range(2):
            for d, perm in enumerate((right, left)):
                if s <= hops[h][d]:
                    cur[h][d] = lax.ppermute(cur[h][d], "tp", perm)
        for h in range(2):
            if s == 1:
                mine, cur[h][0], cur[h][1] = lax.optimization_barrier(
                    (got1[h * half : (h + 1) * half], cur[h][0], cur[h][1])
                )
                acc[h] = gate_up(mine, me * ring_piece, ring_piece)
            if s == far:
                acc[h] = acc[h] + gate_up(got2[h * half : (h + 1) * half], ring_width, flat_width)
            for d in range(2):
                if s <= hops[h][d]:
                    origin = at(-s) if d == 0 else at(s)
                    acc[h] = acc[h] + gate_up(cur[h][d], origin * ring_piece, ring_piece)
    hidden = []
    for h in range(2):
        g = acc[h][:, :hidden_width]
        u = acc[h][:, hidden_width:]
        hidden.append((g / (1.0 + jnp.exp(-g)) * u).astype(jnp.bfloat16))

    wd2 = wd.reshape(wd.shape[0], n_tp, piece)[:, :, ring_piece:].reshape(wd.shape[0], flat_width)
    back2 = f32_dot(jnp.concatenate(hidden, axis=0), wd2).astype(jnp.bfloat16)
    home2 = lax.all_to_all(back2.reshape(n_ep, CAP, flat_width), "ep", 0, 0, tiled=True).reshape(rows, flat_width)

    def down(h, target):
        cols = lax.dynamic_slice_in_dim(wd, target * piece, ring_piece, 1)
        return f32_dot(hidden[h], cols)

    moving = [[None, None], [None, None]]
    for s in range(far, 0, -1):
        for h in range(2):
            for d, perm in enumerate((right, left)):
                if s <= hops[h][d]:
                    target = at(s) if d == 0 else at(-s)
                    part = down(h, target)
                    if moving[h][d] is not None:
                        part = part + moving[h][d].astype(jnp.float32)
                    moving[h][d] = lax.ppermute(part.astype(jnp.bfloat16), "tp", perm)
    back1 = []
    for h in range(2):
        total = down(h, me) + moving[h][0].astype(jnp.float32) + moving[h][1].astype(jnp.float32)
        back1.append(total.astype(jnp.bfloat16))
    back1 = jnp.concatenate(back1, axis=0).reshape(n_ep, CAP, ring_piece)
    home1 = lax.all_to_all(back1, "ep", 0, 0, tiled=True).reshape(rows, ring_piece)

    first_dims = (((0,), (0,)), ((), ()))

    def combine(x):
        return f32_dot(weight_high, x, first_dims) + f32_dot(weight_low, x, first_dims)

    mixed2 = combine(home2).astype(jnp.bfloat16)
    swapped = lax.dynamic_slice_in_dim(mixed2, me * flat_piece, flat_piece, 1).astype(jnp.float32)
    for d in range(1, n_tp):
        theirs = lax.dynamic_slice_in_dim(mixed2, at(d) * flat_piece, flat_piece, 1)
        theirs = lax.ppermute(theirs, "tp", [(i, (i + d) % n_tp) for i in range(n_tp)])
        swapped = swapped + theirs.astype(jnp.float32)
    combined = jnp.concatenate([combine(home1), swapped], axis=1)

    stats = jnp.stack([jnp.sum(combined, axis=1), jnp.sum(combined * combined, axis=1)])
    stats = lax.all_to_all(jnp.broadcast_to(stats[None], (n_tp, *stats.shape)), "tp", 0, 0, tiled=True)
    stats = jnp.sum(stats, axis=0)
    row_mean = stats[0] / D
    row_var = stats[1] / D - row_mean * row_mean
    normed = (combined - row_mean[:, None]) * lax.rsqrt(
        row_var[:, None] + norm_eps
    ) * norm_gain + norm_bias
    return normed.astype(jnp.bfloat16)


def solution(mesh):
    return jax.shard_map(
        layer,
        mesh=mesh,
        in_specs=(
            P(("grp", "ep"), None),
            P(("grp", "ep"), None),
            P(("grp", "ep"), None),
            P("ep", None, "tp"),
            P("ep", None, "tp"),
            P("ep", "tp", None),
            P("tp"),
            P("tp"),
        ),
        out_specs=P(("grp", "ep"), "tp"),
        check_vma=False,
    )
```

```python
import jax
import jax.numpy as jnp
from jax import lax
from jax.sharding import PartitionSpec as P

D = 4096
EXPERTS = 16
CAP = 64
RING_PARTS = 3
ALL_PARTS = 4

norm_eps = 1e-05


def f32_dot(a, b, dims=(((1,), (0,)), ((), ()))):
    return lax.dot_general(a, b, dims, preferred_element_type=jnp.float32)


def route(expert_ids, gates):
    ids = expert_ids.T
    tok = ids.shape[1]
    experts = jnp.arange(EXPERTS, dtype=jnp.int32)[:, None]
    first = ids[0][None, :] == experts
    second = ids[1][None, :] == experts
    named = jnp.logical_or(first, second).astype(jnp.bfloat16)
    row = jnp.arange(tok, dtype=jnp.int32)
    before = (row[:, None] < row[None, :]).astype(jnp.bfloat16)
    slot = f32_dot(named, before).astype(jnp.int32) + experts * CAP
    target0 = jnp.sum(jnp.where(first, slot, 0), axis=0)
    target1 = jnp.sum(jnp.where(second, slot, 0), axis=0)
    slots = jnp.arange(EXPERTS * CAP, dtype=jnp.int32)[:, None]
    at0 = slots == target0[None, :]
    at1 = slots == target1[None, :]
    send = jnp.logical_or(at0, at1).astype(jnp.bfloat16)
    g = gates.T
    weight = jnp.where(at0, g[0][None, :], 0.0) + jnp.where(at1, g[1][None, :], 0.0)
    high = lax.reduce_precision(weight, 8, 7)
    return send, high.astype(jnp.bfloat16), (weight - high).astype(jnp.bfloat16)


def layer(tokens, expert_ids, gates, w_gate, w_up, w_down, norm_gain, norm_bias):
    tok_rows, _ = tokens.shape
    n_tp = lax.axis_size("tp")
    n_ep = lax.axis_size("ep")
    me = lax.axis_index("tp")
    piece = norm_gain.shape[0]
    ring_piece = piece * RING_PARTS // ALL_PARTS
    flat_piece = piece - ring_piece
    ring_width = ring_piece * n_tp
    flat_width = flat_piece * n_tp
    right = [(i, (i + 1) % n_tp) for i in range(n_tp)]
    left = [(i, (i - 1) % n_tp) for i in range(n_tp)]
    far = n_tp // 2

    def at(i):
        return lax.rem(me + i + n_tp, n_tp)

    send, weight_high, weight_low = route(expert_ids, gates)
    own = lax.dynamic_slice_in_dim(tokens, me * ring_piece, ring_piece, 1)
    out1 = f32_dot(send, own).astype(jnp.bfloat16).reshape(n_ep, CAP, ring_piece)
    out2 = f32_dot(send, tokens[:, ring_width:]).astype(jnp.bfloat16).reshape(n_ep, CAP, flat_width)
    got1 = lax.all_to_all(out1, "ep", 0, 0, tiled=True)
    w_both = jnp.concatenate([w_gate[0], w_up[0]], axis=1)
    hidden_width = w_up.shape[2]
    got1, out2, w_both = lax.optimization_barrier((got1, out2, w_both))
    got2 = lax.all_to_all(out2, "ep", 0, 0, tiled=True)

    wd = w_down[0]
    part_rows = CAP // 2
    half = n_ep * part_rows

    def half_of(x, h):
        return x[:, h * part_rows : (h + 1) * part_rows].reshape(half, x.shape[2])

    def gate_up(x, start, size):
        return f32_dot(x, lax.dynamic_slice_in_dim(w_both, start, size, 0))

    hops = ((far, n_tp - 1 - far), (n_tp - 1 - far, far))
    cur = []
    acc = [None, None]
    for h in range(2):
        x = half_of(got1, h)
        cur.append([x, x])
    for s in range(1, far + 1):
        for h in range(2):
            for d, perm in enumerate((right, left)):
                if s <= hops[h][d]:
                    cur[h][d] = lax.ppermute(cur[h][d], "tp", perm)
        for h in range(2):
            if s == 1:
                mine, cur[h][0], cur[h][1] = lax.optimization_barrier(
                    (half_of(got1, h), cur[h][0], cur[h][1])
                )
                acc[h] = gate_up(mine, me * ring_piece, ring_piece)
            if s == far:
                acc[h] = acc[h] + gate_up(half_of(got2, h), ring_width, flat_width)
            for d in range(2):
                if s <= hops[h][d]:
                    origin = at(-s) if d == 0 else at(s)
                    acc[h] = acc[h] + gate_up(cur[h][d], origin * ring_piece, ring_piece)
    hidden = []
    for h in range(2):
        g = acc[h][:, :hidden_width]
        u = acc[h][:, hidden_width:]
        hidden.append((g / (1.0 + jnp.exp(-g)) * u).astype(jnp.bfloat16))

    def down(x, target):
        return f32_dot(x, lax.dynamic_slice_in_dim(wd, target * piece, piece, 1))

    combined = 0.0
    quarter = half // 2
    gone = [[None, None], [None, None]]
    for h in range(2):
        back = []
        for p in range(2):
            x0 = hidden[h][p * quarter : (p + 1) * quarter]
            arrived = []
            for d, perm in enumerate((right, left)):
                x = x0
                if gone[p][d] is not None:
                    x, _ = lax.optimization_barrier((x, gone[p][d]))
                n = hops[p][d]
                seen = []
                for j in range(n):
                    target = at(n - j) if d == 0 else at(j - n)
                    if j == 1:
                        x, _ = lax.optimization_barrier((x, seen[0]))
                    elif j > 1:
                        x, _ = lax.optimization_barrier((x, seen[j - 2]))
                    part = down(x, target)
                    if seen:
                        part = part + seen[-1].astype(jnp.float32)
                    seen.append(lax.ppermute(part.astype(jnp.bfloat16), "tp", perm))
                gone[p][d] = seen[n - 2]
                arrived.append(seen[-1])
                if d == 0:
                    x0, _ = lax.optimization_barrier((x0, seen[n - 2]))
                    last = down(x0, me)
                    x0 = hidden[h][p * quarter : (p + 1) * quarter]
            total = last + arrived[0].astype(jnp.float32) + arrived[1].astype(jnp.float32)
            back.append(total.astype(jnp.bfloat16))
        back = jnp.concatenate(back, axis=0).reshape(n_ep, part_rows, piece)
        home = lax.all_to_all(back, "ep", 0, 0, tiled=True).reshape(half, piece)
        for weight in (weight_high, weight_low):
            weight = half_of(weight.reshape(EXPERTS, CAP, tok_rows), h)
            combined = combined + f32_dot(weight, home, (((0,), (0,)), ((), ())))

    stats = jnp.stack([jnp.sum(combined, axis=1), jnp.sum(combined * combined, axis=1)])
    stats = lax.all_to_all(jnp.broadcast_to(stats[None], (n_tp, *stats.shape)), "tp", 0, 0, tiled=True)
    stats = jnp.sum(stats, axis=0)
    row_mean = stats[0] / D
    row_var = stats[1] / D - row_mean * row_mean
    normed = (combined - row_mean[:, None]) * lax.rsqrt(
        row_var[:, None] + norm_eps
    ) * norm_gain + norm_bias
    return normed.astype(jnp.bfloat16)


def solution(mesh):
    return jax.shard_map(
        layer,
        mesh=mesh,
        in_specs=(
            P(("grp", "ep"), None),
            P(("grp", "ep"), None),
            P(("grp", "ep"), None),
            P("ep", None, "tp"),
            P("ep", None, "tp"),
            P("ep", "tp", None),
            P("tp"),
            P("tp"),
        ),
        out_specs=P(("grp", "ep"), "tp"),
        check_vma=False,
    )
```

```python
import jax
import jax.numpy as jnp
from jax import lax
from jax.sharding import PartitionSpec as P

D = 4096
EXPERTS = 16
CAP = 64
RING_PARTS = 3
ALL_PARTS = 4

norm_eps = 1e-05


def f32_dot(a, b, dims=(((1,), (0,)), ((), ()))):
    return lax.dot_general(a, b, dims, preferred_element_type=jnp.float32)


def route(expert_ids, gates):
    ids = expert_ids.T
    tok = ids.shape[1]
    experts = jnp.arange(EXPERTS, dtype=jnp.int32)[:, None]
    first = ids[0][None, :] == experts
    second = ids[1][None, :] == experts
    named = jnp.logical_or(first, second).astype(jnp.bfloat16)
    row = jnp.arange(tok, dtype=jnp.int32)
    before = (row[:, None] < row[None, :]).astype(jnp.bfloat16)
    slot = f32_dot(named, before).astype(jnp.int32) + experts * CAP
    target0 = jnp.sum(jnp.where(first, slot, 0), axis=0)
    target1 = jnp.sum(jnp.where(second, slot, 0), axis=0)
    slots = jnp.arange(EXPERTS * CAP, dtype=jnp.int32)[:, None]
    at0 = slots == target0[None, :]
    at1 = slots == target1[None, :]
    send = jnp.logical_or(at0, at1).astype(jnp.bfloat16)
    g = gates.T
    weight = jnp.where(at0, g[0][None, :], 0.0) + jnp.where(at1, g[1][None, :], 0.0)
    high = lax.reduce_precision(weight, 8, 7)
    return send, high.astype(jnp.bfloat16), (weight - high).astype(jnp.bfloat16)


def layer(tokens, expert_ids, gates, w_gate, w_up, w_down, norm_gain, norm_bias):
    tok_rows, _ = tokens.shape
    n_tp = lax.axis_size("tp")
    n_ep = lax.axis_size("ep")
    me = lax.axis_index("tp")
    piece = norm_gain.shape[0]
    ring_piece = piece * RING_PARTS // ALL_PARTS
    flat_piece = piece - ring_piece
    ring_width = ring_piece * n_tp
    flat_width = flat_piece * n_tp
    right = [(i, (i + 1) % n_tp) for i in range(n_tp)]
    left = [(i, (i - 1) % n_tp) for i in range(n_tp)]
    far = n_tp // 2

    def at(i):
        return lax.rem(me + i + n_tp, n_tp)

    wd = w_down[0]
    rows = n_ep * CAP
    half = rows // 2
    hidden_width = w_up.shape[2]
    send, weight_high, weight_low = route(expert_ids, gates)
    own = lax.dynamic_slice_in_dim(tokens, me * ring_piece, ring_piece, 1)
    out1 = f32_dot(send, own).astype(jnp.bfloat16).reshape(n_ep, CAP, ring_piece)
    out2 = f32_dot(send, tokens[:, ring_width:]).astype(jnp.bfloat16).reshape(n_ep, CAP, flat_width)
    got1 = lax.all_to_all(out1, "ep", 0, 0, tiled=True).reshape(rows, ring_piece)
    w_both = jnp.concatenate([w_gate[0], w_up[0]], axis=1)
    wd2 = wd.reshape(hidden_width, n_tp, piece)[:, :, ring_piece:].reshape(hidden_width, flat_width)
    got1, out2, w_both, wd2, weight_high, weight_low = lax.optimization_barrier(
        (got1, out2, w_both, wd2, weight_high, weight_low)
    )
    got2 = lax.all_to_all(out2, "ep", 0, 0, tiled=True).reshape(rows, flat_width)

    def gate_up(x, start, size):
        return f32_dot(x, lax.dynamic_slice_in_dim(w_both, start, size, 0))

    to_right = got1
    to_left = got1
    for s in range(1, far):
        to_right = lax.ppermute(to_right, "tp", right)
        to_left = lax.ppermute(to_left, "tp", left)
        if s == 1:
            got1, to_right, to_left = lax.optimization_barrier((got1, to_right, to_left))
            acc = gate_up(got1, me * ring_piece, ring_piece)
        acc = acc + gate_up(to_right, at(-s) * ring_piece, ring_piece)
        acc = acc + gate_up(to_left, at(s) * ring_piece, ring_piece)
    far_top = lax.ppermute(to_right[:half], "tp", right)
    far_bottom = lax.ppermute(to_left[half:], "tp", left)
    acc = acc + gate_up(got2, ring_width, flat_width)
    acc = acc + gate_up(jnp.concatenate([far_top, far_bottom], axis=0), at(far) * ring_piece, ring_piece)
    g = acc[:, :hidden_width]
    u = acc[:, hidden_width:]
    hidden = (g / (1.0 + jnp.exp(-g)) * u).astype(jnp.bfloat16)

    def down(x, target):
        return f32_dot(x, lax.dynamic_slice_in_dim(wd, target * piece, ring_piece, 1))

    farthest = down(hidden, at(far)).astype(jnp.bfloat16)
    to_right = lax.ppermute(farthest[:half], "tp", right)
    to_left = lax.ppermute(farthest[half:], "tp", left)
    back2 = f32_dot(hidden, wd2).astype(jnp.bfloat16)
    home2 = lax.all_to_all(back2.reshape(n_ep, CAP, flat_width), "ep", 0, 0, tiled=True).reshape(rows, flat_width)
    seen_right = [to_right]
    seen_left = [to_left]
    for j in range(1, far + 1):
        s = far - j
        tie = max(j - 2, 0)
        x, seen_right[tie], seen_left[tie] = lax.optimization_barrier((hidden, seen_right[tie], seen_left[tie]))
        from_left = seen_right[-1].astype(jnp.float32)
        from_right = seen_left[-1].astype(jnp.float32)
        if j == 1:
            from_left = jnp.pad(from_left, ((0, half), (0, 0)))
            from_right = jnp.pad(from_right, ((half, 0), (0, 0)))
        if s == 0:
            back1 = (down(x, me) + from_left + from_right).astype(jnp.bfloat16)
            break
        to_right = (down(x, at(s)) + from_left).astype(jnp.bfloat16)
        to_left = (down(x, at(-s)) + from_right).astype(jnp.bfloat16)
        seen_right.append(lax.ppermute(to_right, "tp", right))
        seen_left.append(lax.ppermute(to_left, "tp", left))

    first_dims = (((0,), (0,)), ((), ()))

    def combine(x):
        return f32_dot(weight_high, x, first_dims) + f32_dot(weight_low, x, first_dims)

    mixed2 = combine(home2).astype(jnp.bfloat16).reshape(tok_rows, n_tp, flat_piece)
    mixed2 = lax.all_to_all(mixed2.transpose(1, 0, 2), "tp", 0, 0, tiled=True)
    back1, mixed2 = lax.optimization_barrier((back1, mixed2))
    home1 = lax.all_to_all(back1.reshape(n_ep, CAP, ring_piece), "ep", 0, 0, tiled=True).reshape(rows, ring_piece)
    combined = jnp.concatenate([combine(home1), jnp.sum(mixed2.astype(jnp.float32), axis=0)], axis=1)

    stats = jnp.stack([jnp.sum(combined, axis=1), jnp.sum(combined * combined, axis=1)])
    stats = lax.all_to_all(jnp.broadcast_to(stats[None], (n_tp, *stats.shape)), "tp", 0, 0, tiled=True)
    stats = jnp.sum(stats, axis=0)
    row_mean = stats[0] / D
    row_var = stats[1] / D - row_mean * row_mean
    normed = (combined - row_mean[:, None]) * lax.rsqrt(
        row_var[:, None] + norm_eps
    ) * norm_gain + norm_bias
    return normed.astype(jnp.bfloat16)


def solution(mesh):
    return jax.shard_map(
        layer,
        mesh=mesh,
        in_specs=(
            P(("grp", "ep"), None),
            P(("grp", "ep"), None),
            P(("grp", "ep"), None),
            P("ep", None, "tp"),
            P("ep", None, "tp"),
            P("ep", "tp", None),
            P("tp"),
            P("tp"),
        ),
        out_specs=P(("grp", "ep"), "tp"),
        check_vma=False,
    )
```

```python
import jax
import jax.numpy as jnp
from jax import lax
from jax.experimental import pallas as pl
from jax.sharding import PartitionSpec as P

D = 4096
EXPERTS = 16
CAP = 64
RING_PARTS = 3
ALL_PARTS = 4
GROUPS = 2

norm_eps = 1e-05


def f32_dot(a, b, dims=(((1,), (0,)), ((), ()))):
    return lax.dot_general(a, b, dims, preferred_element_type=jnp.float32)


def route(expert_ids, gates):
    ids = expert_ids.T
    tok = ids.shape[1]
    experts = jnp.arange(EXPERTS, dtype=jnp.int32)[:, None]
    first = ids[0][None, :] == experts
    second = ids[1][None, :] == experts
    named = jnp.logical_or(first, second).astype(jnp.bfloat16)
    row = jnp.arange(tok, dtype=jnp.int32)
    before = (row[:, None] < row[None, :]).astype(jnp.bfloat16)
    slot = f32_dot(named, before).astype(jnp.int32) + experts * CAP
    target0 = jnp.sum(jnp.where(first, slot, 0), axis=0)
    target1 = jnp.sum(jnp.where(second, slot, 0), axis=0)
    slots = jnp.arange(EXPERTS * CAP, dtype=jnp.int32)[:, None]
    at0 = slots == target0[None, :]
    at1 = slots == target1[None, :]
    send = jnp.logical_or(at0, at1).astype(jnp.bfloat16)
    g = gates.T
    weight = jnp.where(at0, g[0][None, :], 0.0) + jnp.where(at1, g[1][None, :], 0.0)
    high = lax.reduce_precision(weight, 8, 7)
    return send, high.astype(jnp.bfloat16), (weight - high).astype(jnp.bfloat16)


def down_kernel(hidden, weights, ring_out, flat_out):
    ring_piece = ring_out.shape[2]
    part = f32_dot(hidden[...], weights[...]).astype(jnp.bfloat16)
    ring_out[0] = part[:, :ring_piece]
    flat_out[...] = part[:, ring_piece:]


def down(hidden, weights, pieces, ring_piece):
    rows, inner = hidden.shape
    piece = weights.shape[1] // pieces
    flat_piece = piece - ring_piece
    return pl.pallas_call(
        down_kernel,
        grid=(pieces,),
        in_specs=[
            pl.BlockSpec((rows, inner), lambda i: (0, 0)),
            pl.BlockSpec((inner, piece), lambda i: (0, i)),
        ],
        out_specs=[
            pl.BlockSpec((1, rows, ring_piece), lambda i: (i, 0, 0)),
            pl.BlockSpec((rows, flat_piece), lambda i: (0, i)),
        ],
        out_shape=[
            jax.ShapeDtypeStruct((pieces, rows, ring_piece), jnp.bfloat16),
            jax.ShapeDtypeStruct((rows, flat_piece * pieces), jnp.bfloat16),
        ],
        cost_estimate=pl.CostEstimate(
            flops=2 * rows * inner * piece * pieces,
            transcendentals=0,
            bytes_accessed=2 * (rows * inner + inner * piece * pieces + rows * piece * pieces),
        ),
        name="down",
    )(hidden, weights)


def layer(tokens, expert_ids, gates, w_gate, w_up, w_down, norm_gain, norm_bias):
    n_tp = lax.axis_size("tp")
    n_ep = lax.axis_size("ep")
    me = lax.axis_index("tp")
    piece = norm_gain.shape[0]
    ring_piece = piece * RING_PARTS // ALL_PARTS
    flat_piece = piece - ring_piece
    ring_width = ring_piece * n_tp
    flat_width = flat_piece * n_tp
    wd = w_down[0]
    part_rows = CAP // GROUPS
    group = n_ep * part_rows
    hidden_width = w_up.shape[2]
    send, weight_high, weight_low = route(expert_ids, gates)
    own = lax.dynamic_slice_in_dim(tokens, me * ring_piece, ring_piece, 1)

    def group_of(x, h):
        return x.reshape(n_ep, CAP, x.shape[-1])[:, h * part_rows : (h + 1) * part_rows].reshape(group, x.shape[-1])

    arrived = []
    for h in range(GROUPS):
        out = f32_dot(group_of(send, h), own).astype(jnp.bfloat16).reshape(n_ep, part_rows, ring_piece)
        arrived.append(lax.all_to_all(out, "ep", 0, 0, tiled=True).reshape(group, ring_piece))
    out = f32_dot(send, tokens[:, ring_width:]).astype(jnp.bfloat16).reshape(n_ep, CAP, flat_width)
    w_both = jnp.concatenate([w_gate[0], w_up[0]], axis=1)
    arrived[-1], out, w_both, weight_high, weight_low = lax.optimization_barrier(
        (arrived[-1], out, w_both, weight_high, weight_low)
    )
    flat = lax.all_to_all(out, "ep", 0, 0, tiled=True)

    whole = []
    for h in range(GROUPS):
        whole.append(lax.all_gather(arrived[h], "tp", axis=1, tiled=True))
    hidden = []
    for h in range(GROUPS):
        acc = f32_dot(whole[h], w_both[:ring_width]) + f32_dot(group_of(flat, h), w_both[ring_width:])
        g = acc[:, :hidden_width]
        u = acc[:, hidden_width:]
        hidden.append((g / (1.0 + jnp.exp(-g)) * u).astype(jnp.bfloat16))

    back = []
    back2 = []
    for x in hidden:
        ring_part, flat_part = down(x, wd, n_tp, ring_piece)
        back.append(ring_part)
        back2.append(flat_part.reshape(n_ep, part_rows, flat_width))
    for h in range(GROUPS - 1):
        back[h], whole[-1] = lax.optimization_barrier((back[h], whole[-1]))
    summed = []
    for h in range(GROUPS):
        summed.append(lax.psum_scatter(back[h], "tp", scatter_dimension=0))
    back2 = jnp.concatenate(back2, axis=1)
    flat = lax.all_to_all(back2, "ep", 0, 0, tiled=True).reshape(n_ep * CAP, flat_width)

    first_dims = (((0,), (0,)), ((), ()))
    mixed2 = f32_dot(weight_high, flat, first_dims) + f32_dot(weight_low, flat, first_dims)
    mixed2 = lax.psum_scatter(mixed2.astype(jnp.bfloat16), "tp", scatter_dimension=1, tiled=True)
    mixed1 = 0.0
    for h in range(GROUPS):
        home = lax.all_to_all(summed[h].reshape(n_ep, part_rows, ring_piece), "ep", 0, 0, tiled=True)
        home = home.reshape(group, ring_piece)
        for weight in (weight_high, weight_low):
            mixed1 = mixed1 + f32_dot(group_of(weight, h), home, first_dims)
    combined = jnp.concatenate([mixed1, mixed2.astype(jnp.float32)], axis=1)

    stats = jnp.stack([jnp.sum(combined, axis=1), jnp.sum(combined * combined, axis=1)])
    stats = lax.all_to_all(jnp.broadcast_to(stats[None], (n_tp, *stats.shape)), "tp", 0, 0, tiled=True)
    stats = jnp.sum(stats, axis=0)
    row_mean = stats[0] / D
    row_var = stats[1] / D - row_mean * row_mean
    normed = (combined - row_mean[:, None]) * lax.rsqrt(
        row_var[:, None] + norm_eps
    ) * norm_gain + norm_bias
    return normed.astype(jnp.bfloat16)


def solution(mesh):
    return jax.shard_map(
        layer,
        mesh=mesh,
        in_specs=(
            P(("grp", "ep"), None),
            P(("grp", "ep"), None),
            P(("grp", "ep"), None),
            P("ep", None, "tp"),
            P("ep", None, "tp"),
            P("ep", "tp", None),
            P("tp"),
            P("tp"),
        ),
        out_specs=P(("grp", "ep"), "tp"),
        check_vma=False,
    )
```

```python
import jax
import jax.numpy as jnp
from jax import lax
from jax.experimental import pallas as pl
from jax.experimental.pallas import tpu as pltpu
from jax.sharding import PartitionSpec as P

D = 4096
EXPERTS = 16
CAP = 64
RING_PARTS = 3
ALL_PARTS = 4
ROW_BLOCK = 128
COLUMN_BLOCK = 128

norm_eps = 1e-05


def f32_dot(a, b, dims=(((1,), (0,)), ((), ()))):
    return lax.dot_general(a, b, dims, preferred_element_type=jnp.float32)


def route(expert_ids, gates):
    ids = expert_ids.T
    tok = ids.shape[1]
    experts = jnp.arange(EXPERTS, dtype=jnp.int32)[:, None]
    first = ids[0][None, :] == experts
    second = ids[1][None, :] == experts
    named = jnp.logical_or(first, second).astype(jnp.bfloat16)
    row = jnp.arange(tok, dtype=jnp.int32)
    before = (row[:, None] < row[None, :]).astype(jnp.bfloat16)
    slot = f32_dot(named, before).astype(jnp.int32) + experts * CAP
    target0 = jnp.sum(jnp.where(first, slot, 0), axis=0)
    target1 = jnp.sum(jnp.where(second, slot, 0), axis=0)
    slots = jnp.arange(EXPERTS * CAP, dtype=jnp.int32)[:, None]
    at0 = slots == target0[None, :]
    at1 = slots == target1[None, :]
    send = jnp.logical_or(at0, at1).astype(jnp.bfloat16)
    g = gates.T
    weight = jnp.where(at0, g[0][None, :], 0.0) + jnp.where(at1, g[1][None, :], 0.0)
    high = lax.reduce_precision(weight, 8, 7)
    return send, high.astype(jnp.bfloat16), (weight - high).astype(jnp.bfloat16)


def by_rows(shape, first=0):
    return pl.BlockSpec((ROW_BLOCK, shape[1]), lambda i, index: (i + first // ROW_BLOCK, 0))


def gate_up(acc, parts, w_gate, w_up, rows, finish):
    count = len(parts)
    width = w_gate.shape[1]

    def kernel(index_ref, *refs):
        out = refs[-1]
        xs = refs[:count]
        gates = refs[count : 2 * count]
        ups = refs[2 * count : 3 * count]
        g = 0.0
        u = 0.0
        for x, wg, wu in zip(xs, gates, ups):
            g = g + f32_dot(x[...], wg[...])
            u = u + f32_dot(x[...], wu[...])
        if acc is not None:
            g = g + refs[3 * count][:, :width]
            u = u + refs[3 * count][:, width:]
        if finish:
            out[...] = (g / (1.0 + jnp.exp(-g)) * u).astype(out.dtype)
        else:
            out[:, :width] = g
            out[:, width:] = u

    def weight_spec(k):
        return pl.BlockSpec((parts[k][0].shape[1], width), lambda i, index: (index[k], 0))

    specs = [by_rows(x.shape, first) for x, _, first in parts]
    specs += [weight_spec(k) for k in range(count)] * 2
    operands = [x for x, _, _ in parts] + [w_gate] * count + [w_up] * count
    if acc is not None:
        specs.append(by_rows(acc.shape))
        operands.append(acc)
    inner = sum(x.shape[1] for x, _, _ in parts)
    out_shape = (rows, width) if finish else (rows, 2 * width)
    return pl.pallas_call(
        kernel,
        grid_spec=pltpu.PrefetchScalarGridSpec(
            num_scalar_prefetch=1, grid=(rows // ROW_BLOCK,), in_specs=specs, out_specs=by_rows(out_shape)
        ),
        out_shape=jax.ShapeDtypeStruct(out_shape, jnp.bfloat16 if finish else jnp.float32),
        cost_estimate=pl.CostEstimate(
            flops=4 * rows * inner * width, transcendentals=0, bytes_accessed=2 * inner * (rows + 2 * width)
        ),
        name="gate_up",
    )(jnp.stack([jnp.asarray(i, jnp.int32) for _, i, _ in parts]), *operands)


def down(hidden, w_down, target, piece, keep, others):
    count = len(hidden)
    rows, inner = hidden[0].shape

    def kernel(index_ref, *refs):
        out = refs[-1]
        each = (len(refs) - 2 - count) // count
        for h in range(count):
            total = f32_dot(refs[h][...], refs[count][:, :keep])
            for ref in refs[count + 1 + h * each : count + 1 + (h + 1) * each]:
                total = total + ref[...].astype(jnp.float32)
            out[h] = total.astype(jnp.bfloat16)

    return pl.pallas_call(
        kernel,
        grid_spec=pltpu.PrefetchScalarGridSpec(
            num_scalar_prefetch=1,
            grid=(rows // ROW_BLOCK,),
            in_specs=[by_rows(x.shape) for x in hidden]
            + [pl.BlockSpec((inner, piece), lambda i, index: (0, index[0]))]
            + [by_rows(x.shape) for x in others],
            out_specs=pl.BlockSpec((count, ROW_BLOCK, keep), lambda i, index: (0, i, 0)),
        ),
        out_shape=jax.ShapeDtypeStruct((count, rows, keep), jnp.bfloat16),
        cost_estimate=pl.CostEstimate(
            flops=2 * count * rows * inner * keep, transcendentals=0, bytes_accessed=4 * count * rows * keep
        ),
        name="down",
    )(jnp.reshape(target, (1,)).astype(jnp.int32), *hidden, w_down, *others)


def flat_down(hidden, w_down, pieces, keep):
    rows, inner = hidden[0].shape
    count = len(hidden)
    piece = w_down.shape[1] // pieces
    rest = piece - keep

    def kernel(*refs):
        for h in range(count):
            refs[-1][h] = f32_dot(refs[h][...], refs[count][:, keep:]).astype(jnp.bfloat16)

    def place(i):
        where = 0
        step = 1
        while step < pieces:
            where = where * 2 + (i // step) % 2
            step *= 2
        return (0, 0, where)

    return pl.pallas_call(
        kernel,
        grid=(pieces,),
        in_specs=[pl.BlockSpec((rows, inner), lambda i: (0, 0))] * count
        + [pl.BlockSpec((inner, piece), lambda i: (0, i))],
        out_specs=pl.BlockSpec((count, rows, rest), place),
        out_shape=jax.ShapeDtypeStruct((count, rows, rest * pieces), jnp.bfloat16),
        cost_estimate=pl.CostEstimate(
            flops=2 * count * rows * inner * rest * pieces, transcendentals=0, bytes_accessed=4 * count * rows * rest * pieces
        ),
        name="flat_down",
    )(*hidden, w_down)


def mix(weights, x, tokens):
    rows, width = x.shape

    def kernel(w, x, out):
        both = f32_dot(w[...], x[...], (((0,), (0,)), ((), ())))
        out[...] = both[:tokens] + both[tokens:]

    return pl.pallas_call(
        kernel,
        grid=(width // COLUMN_BLOCK,),
        in_specs=[
            pl.BlockSpec(weights.shape, lambda i: (0, 0)),
            pl.BlockSpec((rows, COLUMN_BLOCK), lambda i: (0, i)),
        ],
        out_specs=pl.BlockSpec((tokens, COLUMN_BLOCK), lambda i: (0, i)),
        out_shape=jax.ShapeDtypeStruct((tokens, width), jnp.float32),
        cost_estimate=pl.CostEstimate(
            flops=2 * weights.size * width, transcendentals=0, bytes_accessed=2 * x.size + 4 * tokens * width
        ),
        name="mix",
    )(weights, x)


def dispatch(send, tokens, first, width):
    rows, tok = send.shape

    def kernel(index_ref, w, x, out):
        out[...] = f32_dot(w[...], x[...]).astype(jnp.bfloat16)

    return pl.pallas_call(
        kernel,
        grid_spec=pltpu.PrefetchScalarGridSpec(
            num_scalar_prefetch=1,
            grid=(width // COLUMN_BLOCK,),
            in_specs=[
                pl.BlockSpec((rows, tok), lambda i, index: (0, 0)),
                pl.BlockSpec((tok, COLUMN_BLOCK), lambda i, index: (0, index[0] + i)),
            ],
            out_specs=pl.BlockSpec((rows, COLUMN_BLOCK), lambda i, index: (0, i)),
        ),
        out_shape=jax.ShapeDtypeStruct((rows, width), jnp.bfloat16),
        cost_estimate=pl.CostEstimate(
            flops=2 * rows * tok * width, transcendentals=0, bytes_accessed=2 * (rows + tok) * width
        ),
        name="dispatch",
    )(jnp.asarray(first // COLUMN_BLOCK, jnp.int32).reshape(1), send, tokens)


def layer(tokens, expert_ids, gates, w_gate, w_up, w_down, norm_gain, norm_bias):
    tok_rows, _ = tokens.shape
    n_tp = lax.axis_size("tp")
    n_ep = lax.axis_size("ep")
    me = lax.axis_index("tp")
    piece = norm_gain.shape[0]
    ring_piece = piece * RING_PARTS // ALL_PARTS
    flat_piece = piece - ring_piece
    ring_width = ring_piece * n_tp
    flat_width = flat_piece * n_tp
    right = [(i, (i + 1) % n_tp) for i in range(n_tp)]
    left = [(i, (i - 1) % n_tp) for i in range(n_tp)]
    far = n_tp // 2

    def at(i):
        return lax.rem(me + i + n_tp, n_tp)

    wg = w_gate[0]
    wu = w_up[0]
    wd = w_down[0]
    rows = n_ep * CAP
    half = rows // 2
    send, weight_high, weight_low = route(expert_ids, gates)
    out1 = dispatch(send, tokens, me * ring_piece, ring_piece).reshape(n_ep, CAP, ring_piece)
    out2 = dispatch(send, tokens, ring_width, flat_width).reshape(n_ep, CAP, flat_width)
    got1 = lax.all_to_all(out1, "ep", 0, 0, tiled=True).reshape(rows, ring_piece)
    weights = jnp.concatenate([weight_high, weight_low], axis=1)
    got1, out2, weights = lax.optimization_barrier((got1, out2, weights))
    got2 = lax.all_to_all(out2, "ep", 0, 0, tiled=True).reshape(rows, flat_width)

    hops = ((far, n_tp - 1 - far), (n_tp - 1 - far, far))
    cur = []
    acc = [None, None]
    parts = [[], []]
    for h in range(2):
        x = got1[h * half : (h + 1) * half]
        cur.append([x, x])
    for s in range(1, far + 1):
        for h in range(2):
            for d, perm in enumerate((right, left)):
                if s <= hops[h][d]:
                    cur[h][d] = lax.ppermute(cur[h][d], "tp", perm)
        for h in range(2):
            if s == 1:
                mine, cur[h][0], cur[h][1] = lax.optimization_barrier((got1, cur[h][0], cur[h][1]))
                parts[h].append((mine, me, h * half))
            for d in range(2):
                if s <= hops[h][d]:
                    parts[h].append((cur[h][d], at(-s) if d == 0 else at(s), 0))
            if s == far - 1:
                parts[h].append((got2, ring_width // flat_width, h * half))
            if s > 1:
                acc[h] = gate_up(acc[h], parts[h], wg, wu, half, s == far)
                parts[h] = []
    hidden = acc

    moving = [[None, None], [None, None]]
    for s in range(far, 0, -1):
        for h in range(2):
            for d, perm in enumerate((right, left)):
                if s <= hops[h][d]:
                    target = at(s) if d == 0 else at(-s)
                    others = [] if moving[h][d] is None else [moving[h][d]]
                    part = down([hidden[h]], wd, target, piece, ring_piece, others)[0]
                    moving[h][d] = lax.ppermute(part, "tp", perm)
    back1 = down(hidden, wd, me, piece, ring_piece, moving[0] + moving[1]).reshape(n_ep, CAP, ring_piece)
    back2 = flat_down(hidden, wd, n_tp, ring_piece)
    home2 = lax.all_to_all(back2.reshape(n_ep, CAP, flat_width), "ep", 0, 0, tiled=True).reshape(rows, flat_width)
    home1 = lax.all_to_all(back1, "ep", 0, 0, tiled=True).reshape(rows, ring_piece)

    def combine(x):
        return mix(weights, x, tok_rows)

    mixed2 = combine(home2)
    step = 1
    while step < n_tp:
        size = mixed2.shape[1] // 2
        bit = lax.rem(me // step, 2)
        kept = lax.dynamic_slice_in_dim(mixed2, bit * size, size, 1)
        sent = lax.dynamic_slice_in_dim(mixed2, (1 - bit) * size, size, 1).astype(jnp.bfloat16)
        sent = lax.ppermute(sent, "tp", [(i, i ^ step) for i in range(n_tp)])
        mixed2 = kept + sent.astype(jnp.float32)
        step *= 2
    combined = jnp.concatenate([combine(home1), mixed2], axis=1)

    stats = jnp.stack([jnp.sum(combined, axis=1), jnp.sum(combined * combined, axis=1)])
    stats = lax.all_to_all(jnp.broadcast_to(stats[None], (n_tp, *stats.shape)), "tp", 0, 0, tiled=True)
    stats = jnp.sum(stats, axis=0)
    row_mean = stats[0] / D
    row_var = stats[1] / D - row_mean * row_mean
    normed = (combined - row_mean[:, None]) * lax.rsqrt(
        row_var[:, None] + norm_eps
    ) * norm_gain + norm_bias
    return normed.astype(jnp.bfloat16)


def solution(mesh):
    return jax.shard_map(
        layer,
        mesh=mesh,
        in_specs=(
            P(("grp", "ep"), None),
            P(("grp", "ep"), None),
            P(("grp", "ep"), None),
            P("ep", None, "tp"),
            P("ep", None, "tp"),
            P("ep", "tp", None),
            P("tp"),
            P("tp"),
        ),
        out_specs=P(("grp", "ep"), "tp"),
        check_vma=False,
    )
```

```python
import jax
import jax.numpy as jnp
from jax import lax
from jax.sharding import PartitionSpec as P

D = 4096
EXPERTS = 16
CAP = 64
RING_PARTS = 3
ALL_PARTS = 4

norm_eps = 1e-05


def f32_dot(a, b, dims=(((1,), (0,)), ((), ()))):
    return lax.dot_general(a, b, dims, preferred_element_type=jnp.float32)


def route(expert_ids, gates):
    ids = expert_ids.T
    tok = ids.shape[1]
    experts = jnp.arange(EXPERTS, dtype=jnp.int32)[:, None]
    first = ids[0][None, :] == experts
    second = ids[1][None, :] == experts
    named = jnp.logical_or(first, second).astype(jnp.bfloat16)
    row = jnp.arange(tok, dtype=jnp.int32)
    before = (row[:, None] < row[None, :]).astype(jnp.bfloat16)
    slot = f32_dot(named, before).astype(jnp.int32) + experts * CAP
    target0 = jnp.sum(jnp.where(first, slot, 0), axis=0)
    target1 = jnp.sum(jnp.where(second, slot, 0), axis=0)
    slots = jnp.arange(EXPERTS * CAP, dtype=jnp.int32)[:, None]
    at0 = slots == target0[None, :]
    at1 = slots == target1[None, :]
    send = jnp.logical_or(at0, at1).astype(jnp.bfloat16)
    g = gates.T
    weight = jnp.where(at0, g[0][None, :], 0.0) + jnp.where(at1, g[1][None, :], 0.0)
    high = lax.reduce_precision(weight, 8, 7)
    return send, high.astype(jnp.bfloat16), (weight - high).astype(jnp.bfloat16)


def halving_order(count):
    order = [0]
    step = count // 2
    while step:
        order = order + [i + step for i in order]
        step //= 2
    return order


def layer(tokens, expert_ids, gates, w_gate, w_up, w_down, norm_gain, norm_bias):
    n_tp = lax.axis_size("tp")
    n_ep = lax.axis_size("ep")
    me = lax.axis_index("tp")
    piece = norm_gain.shape[0]
    ring_piece = piece * RING_PARTS // ALL_PARTS
    flat_piece = piece - ring_piece
    ring_width = ring_piece * n_tp
    flat_width = flat_piece * n_tp
    right = [(i, (i + 1) % n_tp) for i in range(n_tp)]
    left = [(i, (i - 1) % n_tp) for i in range(n_tp)]
    far = n_tp // 2

    def at(i):
        return lax.rem(me + i + n_tp, n_tp)

    send, weight_high, weight_low = route(expert_ids, gates)
    own = lax.dynamic_slice_in_dim(tokens, me * ring_piece, ring_piece, 1)
    out1 = f32_dot(send, own).astype(jnp.bfloat16).reshape(n_ep, CAP, ring_piece)
    out2 = f32_dot(send, tokens[:, ring_width:]).astype(jnp.bfloat16).reshape(n_ep, CAP, flat_width)
    got1 = lax.all_to_all(out1, "ep", 0, 0, tiled=True).reshape(n_ep * CAP, ring_piece)
    w_both = jnp.concatenate([w_gate[0], w_up[0]], axis=1)
    hidden_width = w_up.shape[2]
    wd = w_down[0]
    wd2 = jnp.concatenate(
        [wd[:, i * piece + ring_piece : (i + 1) * piece] for i in halving_order(n_tp)], axis=1
    )
    got1, out2, w_both, wd2, weight_high, weight_low = lax.optimization_barrier(
        (got1, out2, w_both, wd2, weight_high, weight_low)
    )
    got2 = lax.all_to_all(out2, "ep", 0, 0, tiled=True).reshape(n_ep * CAP, flat_width)

    rows = n_ep * CAP
    half = rows // 2

    def gate_up(x, start, size):
        return f32_dot(x, lax.dynamic_slice_in_dim(w_both, start, size, 0))

    hops = ((far, n_tp - 1 - far), (n_tp - 1 - far, far))
    cur = []
    acc = []
    for h in range(2):
        x = got1[h * half : (h + 1) * half]
        cur.append([x, x])
        acc.append(None)
    for s in range(1, far + 1):
        for h in range(2):
            for d, perm in enumerate((right, left)):
                if s <= hops[h][d]:
                    cur[h][d] = lax.ppermute(cur[h][d], "tp", perm)
        for h in range(2):
            if s == 1:
                mine, cur[h][0], cur[h][1] = lax.optimization_barrier(
                    (got1[h * half : (h + 1) * half], cur[h][0], cur[h][1])
                )
                acc[h] = gate_up(mine, me * ring_piece, ring_piece)
            if s == far:
                acc[h] = acc[h] + gate_up(got2[h * half : (h + 1) * half], ring_width, flat_width)
            for d in range(2):
                if s <= hops[h][d]:
                    origin = at(-s) if d == 0 else at(s)
                    acc[h] = acc[h] + gate_up(cur[h][d], origin * ring_piece, ring_piece)
    hidden = []
    for h in range(2):
        g = acc[h][:, :hidden_width]
        u = acc[h][:, hidden_width:]
        hidden.append((g / (1.0 + jnp.exp(-g)) * u).astype(jnp.bfloat16))

    back2 = f32_dot(jnp.concatenate(hidden, axis=0), wd2).astype(jnp.bfloat16)
    home2 = lax.all_to_all(back2.reshape(n_ep, CAP, flat_width), "ep", 0, 0, tiled=True).reshape(rows, flat_width)

    def down(x, target):
        return f32_dot(x, lax.dynamic_slice_in_dim(wd, target * piece, ring_piece, 1))

    seen = [[[], []], [[], []]]
    for s in range(far, 0, -1):
        for h in range(2):
            for d, perm in enumerate((right, left)):
                if s <= hops[h][d]:
                    target = at(s) if d == 0 else at(-s)
                    so_far = seen[h][d]
                    x = hidden[h]
                    if so_far:
                        tie = max(len(so_far) - 2, 0)
                        x, so_far[tie] = lax.optimization_barrier((x, so_far[tie]))
                    part = down(x, target)
                    if so_far:
                        part = part + so_far[-1].astype(jnp.float32)
                    so_far.append(lax.ppermute(part.astype(jnp.bfloat16), "tp", perm))
    back1 = []
    for h in range(2):
        x, seen[h][0][-2] = lax.optimization_barrier((hidden[h], seen[h][0][-2]))
        total = down(x, me) + seen[h][0][-1].astype(jnp.float32) + seen[h][1][-1].astype(jnp.float32)
        back1.append(total.astype(jnp.bfloat16))
    back1 = jnp.concatenate(back1, axis=0).reshape(n_ep, CAP, ring_piece)
    home1 = lax.all_to_all(back1, "ep", 0, 0, tiled=True).reshape(rows, ring_piece)

    first_dims = (((0,), (0,)), ((), ()))

    def combine(x):
        return f32_dot(weight_high, x, first_dims) + f32_dot(weight_low, x, first_dims)

    mixed2 = combine(home2)
    step = 1
    while step < n_tp:
        size = mixed2.shape[1] // 2
        bit = lax.rem(me // step, 2)
        kept = lax.dynamic_slice_in_dim(mixed2, bit * size, size, 1)
        sent = lax.dynamic_slice_in_dim(mixed2, (1 - bit) * size, size, 1).astype(jnp.bfloat16)
        sent = lax.ppermute(sent, "tp", [(i, i ^ step) for i in range(n_tp)])
        mixed2 = kept + sent.astype(jnp.float32)
        step *= 2
    combined = jnp.concatenate([combine(home1), mixed2], axis=1)

    stats = jnp.stack([jnp.sum(combined, axis=1), jnp.sum(combined * combined, axis=1)])
    stats = lax.all_to_all(jnp.broadcast_to(stats[None], (n_tp, *stats.shape)), "tp", 0, 0, tiled=True)
    stats = jnp.sum(stats, axis=0)
    row_mean = stats[0] / D
    row_var = stats[1] / D - row_mean * row_mean
    normed = (combined - row_mean[:, None]) * lax.rsqrt(
        row_var[:, None] + norm_eps
    ) * norm_gain + norm_bias
    return normed.astype(jnp.bfloat16)


def solution(mesh):
    return jax.shard_map(
        layer,
        mesh=mesh,
        in_specs=(
            P(("grp", "ep"), None),
            P(("grp", "ep"), None),
            P(("grp", "ep"), None),
            P("ep", None, "tp"),
            P("ep", None, "tp"),
            P("ep", "tp", None),
            P("tp"),
            P("tp"),
        ),
        out_specs=P(("grp", "ep"), "tp"),
        check_vma=False,
    )
```

```python
import jax
import jax.numpy as jnp
from jax import lax
from jax.sharding import PartitionSpec as P

D = 4096
EXPERTS = 16
CAP = 64
RING_PARTS = 3
ALL_PARTS = 4

norm_eps = 1e-05


def f32_dot(a, b, dims=(((1,), (0,)), ((), ()))):
    return lax.dot_general(a, b, dims, preferred_element_type=jnp.float32)


def route(expert_ids, gates):
    ids = expert_ids.T
    tok = ids.shape[1]
    experts = jnp.arange(EXPERTS, dtype=jnp.int32)[:, None]
    first = ids[0][None, :] == experts
    second = ids[1][None, :] == experts
    named = jnp.logical_or(first, second).astype(jnp.bfloat16)
    row = jnp.arange(tok, dtype=jnp.int32)
    before = (row[:, None] < row[None, :]).astype(jnp.bfloat16)
    slot = f32_dot(named, before).astype(jnp.int32) + experts * CAP
    target0 = jnp.sum(jnp.where(first, slot, 0), axis=0)
    target1 = jnp.sum(jnp.where(second, slot, 0), axis=0)
    slots = jnp.arange(EXPERTS * CAP, dtype=jnp.int32)[:, None]
    at0 = slots == target0[None, :]
    at1 = slots == target1[None, :]
    send = jnp.logical_or(at0, at1).astype(jnp.bfloat16)
    g = gates.T
    weight = jnp.where(at0, g[0][None, :], 0.0) + jnp.where(at1, g[1][None, :], 0.0)
    high = lax.reduce_precision(weight, 8, 7)
    return send, high.astype(jnp.bfloat16), (weight - high).astype(jnp.bfloat16)


def layer(tokens, expert_ids, gates, w_gate, w_up, w_down, norm_gain, norm_bias):
    n_tp = lax.axis_size("tp")
    n_ep = lax.axis_size("ep")
    me = lax.axis_index("tp")
    piece = norm_gain.shape[0]
    ring_piece = piece * RING_PARTS // ALL_PARTS
    flat_piece = piece - ring_piece
    ring_width = ring_piece * n_tp
    flat_width = flat_piece * n_tp
    right = [(i, (i + 1) % n_tp) for i in range(n_tp)]
    left = [(i, (i - 1) % n_tp) for i in range(n_tp)]
    far = n_tp // 2

    def at(i):
        return lax.rem(me + i + n_tp, n_tp)

    send, weight_high, weight_low = route(expert_ids, gates)
    own = lax.dynamic_slice_in_dim(tokens, me * ring_piece, ring_piece, 1)
    out1 = f32_dot(send, own).astype(jnp.bfloat16).reshape(n_ep, CAP, ring_piece)
    out2 = f32_dot(send, tokens[:, ring_width:]).astype(jnp.bfloat16).reshape(n_ep, CAP, flat_width)
    got1 = lax.all_to_all(out1, "ep", 0, 0, tiled=True).reshape(n_ep * CAP, ring_piece)
    w_both = jnp.concatenate([w_gate[0], w_up[0]], axis=1)
    hidden_width = w_up.shape[2]
    wd = w_down[0]
    bits = n_tp.bit_length() - 1
    wd2 = wd.reshape(hidden_width, *([2] * bits), piece)[..., ring_piece:]
    wd2 = wd2.transpose(0, *range(bits, 0, -1), bits + 1).reshape(hidden_width, flat_width)
    got1, out2, w_both, wd2, weight_high, weight_low = lax.optimization_barrier(
        (got1, out2, w_both, wd2, weight_high, weight_low)
    )
    got2 = lax.all_to_all(out2, "ep", 0, 0, tiled=True).reshape(n_ep * CAP, flat_width)

    rows = n_ep * CAP
    half = rows // 2

    def gate_up(x, start, size):
        return f32_dot(x, lax.dynamic_slice_in_dim(w_both, start, size, 0))

    hops = ((far, n_tp - 1 - far), (n_tp - 1 - far, far))
    cur = []
    acc = []
    for h in range(2):
        x = got1[h * half : (h + 1) * half]
        cur.append([x, x])
        acc.append(None)
    for s in range(1, far + 1):
        for h in range(2):
            for d, perm in enumerate((right, left)):
                if s <= hops[h][d]:
                    cur[h][d] = lax.ppermute(cur[h][d], "tp", perm)
        for h in range(2):
            if s == 1:
                mine, cur[h][0], cur[h][1] = lax.optimization_barrier(
                    (got1[h * half : (h + 1) * half], cur[h][0], cur[h][1])
                )
                acc[h] = gate_up(mine, me * ring_piece, ring_piece)
            if s == far:
                acc[h] = acc[h] + gate_up(got2[h * half : (h + 1) * half], ring_width, flat_width)
            for d in range(2):
                if s <= hops[h][d]:
                    origin = at(-s) if d == 0 else at(s)
                    acc[h] = acc[h] + gate_up(cur[h][d], origin * ring_piece, ring_piece)
    hidden = []
    for h in range(2):
        g = acc[h][:, :hidden_width]
        u = acc[h][:, hidden_width:]
        hidden.append((g / (1.0 + jnp.exp(-g)) * u).astype(jnp.bfloat16))

    back2 = f32_dot(jnp.concatenate(hidden, axis=0), wd2).astype(jnp.bfloat16)
    home2 = lax.all_to_all(back2.reshape(n_ep, CAP, flat_width), "ep", 0, 0, tiled=True).reshape(rows, flat_width)

    def down(x, target):
        return f32_dot(x, lax.dynamic_slice_in_dim(wd, target * piece, ring_piece, 1))

    seen = [[[], []], [[], []]]
    for s in range(far, 0, -1):
        for h in range(2):
            for d, perm in enumerate((right, left)):
                if s <= hops[h][d]:
                    target = at(s) if d == 0 else at(-s)
                    so_far = seen[h][d]
                    x = hidden[h]
                    if so_far:
                        tie = max(len(so_far) - 2, 0)
                        x, so_far[tie] = lax.optimization_barrier((x, so_far[tie]))
                    part = down(x, target)
                    if so_far:
                        part = part + so_far[-1].astype(jnp.float32)
                    so_far.append(lax.ppermute(part.astype(jnp.bfloat16), "tp", perm))
    back1 = []
    for h in range(2):
        x, seen[h][0][-2] = lax.optimization_barrier((hidden[h], seen[h][0][-2]))
        total = down(x, me) + seen[h][0][-1].astype(jnp.float32) + seen[h][1][-1].astype(jnp.float32)
        back1.append(total.astype(jnp.bfloat16))
    back1 = jnp.concatenate(back1, axis=0).reshape(n_ep, CAP, ring_piece)
    home1 = lax.all_to_all(back1, "ep", 0, 0, tiled=True).reshape(rows, ring_piece)

    first_dims = (((0,), (0,)), ((), ()))

    def combine(x):
        return f32_dot(weight_high, x, first_dims) + f32_dot(weight_low, x, first_dims)

    mixed2 = combine(home2)
    step = 1
    while step < n_tp:
        size = mixed2.shape[1] // 2
        bit = lax.rem(me // step, 2)
        kept = lax.dynamic_slice_in_dim(mixed2, bit * size, size, 1)
        sent = lax.dynamic_slice_in_dim(mixed2, (1 - bit) * size, size, 1).astype(jnp.bfloat16)
        sent = lax.ppermute(sent, "tp", [(i, i ^ step) for i in range(n_tp)])
        mixed2 = kept + sent.astype(jnp.float32)
        step *= 2
    combined = jnp.concatenate([combine(home1), mixed2], axis=1)

    stats = jnp.stack([jnp.sum(combined, axis=1), jnp.sum(combined * combined, axis=1)])
    stats = lax.all_to_all(jnp.broadcast_to(stats[None], (n_tp, *stats.shape)), "tp", 0, 0, tiled=True)
    stats = jnp.sum(stats, axis=0)
    row_mean = stats[0] / D
    row_var = stats[1] / D - row_mean * row_mean
    normed = (combined - row_mean[:, None]) * lax.rsqrt(
        row_var[:, None] + norm_eps
    ) * norm_gain + norm_bias
    return normed.astype(jnp.bfloat16)


def solution(mesh):
    return jax.shard_map(
        layer,
        mesh=mesh,
        in_specs=(
            P(("grp", "ep"), None),
            P(("grp", "ep"), None),
            P(("grp", "ep"), None),
            P("ep", None, "tp"),
            P("ep", None, "tp"),
            P("ep", "tp", None),
            P("tp"),
            P("tp"),
        ),
        out_specs=P(("grp", "ep"), "tp"),
        check_vma=False,
    )
```

```python
import jax
import jax.numpy as jnp
from jax import lax
from jax.sharding import PartitionSpec as P

D = 4096
EXPERTS = 16
CAP = 64
RING_PARTS = 3
ALL_PARTS = 4

norm_eps = 1e-05


def f32_dot(a, b, dims=(((1,), (0,)), ((), ()))):
    return lax.dot_general(a, b, dims, preferred_element_type=jnp.float32)


def route(expert_ids, gates):
    ids = expert_ids.T
    tok = ids.shape[1]
    experts = jnp.arange(EXPERTS, dtype=jnp.int32)[:, None]
    first = ids[0][None, :] == experts
    second = ids[1][None, :] == experts
    named = jnp.logical_or(first, second).astype(jnp.bfloat16)
    row = jnp.arange(tok, dtype=jnp.int32)
    before = (row[:, None] < row[None, :]).astype(jnp.bfloat16)
    slot = f32_dot(named, before).astype(jnp.int32) + experts * CAP
    target0 = jnp.sum(jnp.where(first, slot, 0), axis=0)
    target1 = jnp.sum(jnp.where(second, slot, 0), axis=0)
    slots = jnp.arange(EXPERTS * CAP, dtype=jnp.int32)[:, None]
    at0 = slots == target0[None, :]
    at1 = slots == target1[None, :]
    send = jnp.logical_or(at0, at1).astype(jnp.bfloat16)
    g = gates.T
    weight = jnp.where(at0, g[0][None, :], 0.0) + jnp.where(at1, g[1][None, :], 0.0)
    high = lax.reduce_precision(weight, 8, 7)
    return send, high.astype(jnp.bfloat16), (weight - high).astype(jnp.bfloat16)


def layer(tokens, expert_ids, gates, w_gate, w_up, w_down, norm_gain, norm_bias):
    n_tp = lax.axis_size("tp")
    n_ep = lax.axis_size("ep")
    me = lax.axis_index("tp")
    piece = norm_gain.shape[0]
    ring_piece = piece * RING_PARTS // ALL_PARTS
    flat_piece = piece - ring_piece
    ring_width = ring_piece * n_tp
    flat_width = flat_piece * n_tp
    right = [(i, (i + 1) % n_tp) for i in range(n_tp)]
    left = [(i, (i - 1) % n_tp) for i in range(n_tp)]
    far = n_tp // 2

    def at(i):
        return lax.rem(me + i + n_tp, n_tp)

    send, weight_high, weight_low = route(expert_ids, gates)
    own = lax.dynamic_slice_in_dim(tokens, me * ring_piece, ring_piece, 1)
    out1 = f32_dot(send, own).astype(jnp.bfloat16).reshape(n_ep, CAP, ring_piece)
    out2 = f32_dot(send, tokens[:, ring_width:]).astype(jnp.bfloat16).reshape(n_ep, CAP, flat_width)
    got1 = lax.all_to_all(out1, "ep", 0, 0, tiled=True).reshape(n_ep * CAP, ring_piece)
    w_both = jnp.concatenate([w_gate[0], w_up[0]], axis=1)
    hidden_width = w_up.shape[2]
    wd = w_down[0]
    bits = n_tp.bit_length() - 1
    wd2 = wd.reshape(hidden_width, *([2] * bits), piece)[..., ring_piece:]
    wd2 = wd2.transpose(0, *range(bits, 0, -1), bits + 1).reshape(hidden_width, flat_width)
    got1, out2, w_both, wd2, weight_high, weight_low = lax.optimization_barrier(
        (got1, out2, w_both, wd2, weight_high, weight_low)
    )
    got2 = lax.all_to_all(out2, "ep", 0, 0, tiled=True).reshape(n_ep * CAP, flat_width)

    rows = n_ep * CAP
    half = rows // 2

    def gate_up(x, start, size):
        return f32_dot(x, lax.dynamic_slice_in_dim(w_both, start, size, 0))

    hops = ((far, n_tp - 1 - far), (n_tp - 1 - far, far))
    to_right = got1
    to_left = got1
    for s in range(1, far):
        to_right = lax.ppermute(to_right, "tp", right)
        to_left = lax.ppermute(to_left, "tp", left)
        if s == 1:
            got1, to_right, to_left = lax.optimization_barrier((got1, to_right, to_left))
            acc = gate_up(got1, me * ring_piece, ring_piece)
        acc = acc + gate_up(to_right, at(-s) * ring_piece, ring_piece)
        acc = acc + gate_up(to_left, at(s) * ring_piece, ring_piece)
        if s == 2:
            acc = lax.optimization_barrier(acc)
    far_parts = (lax.ppermute(to_right[:half], "tp", right), lax.ppermute(to_left[half:], "tp", left))
    acc = lax.optimization_barrier(acc + gate_up(got2, ring_width, flat_width))
    acc = [
        acc[h * half : (h + 1) * half] + gate_up(far_parts[h], at(far) * ring_piece, ring_piece)
        for h in range(2)
    ]
    hidden = []
    for h in range(2):
        g = acc[h][:, :hidden_width]
        u = acc[h][:, hidden_width:]
        hidden.append((g / (1.0 + jnp.exp(-g)) * u).astype(jnp.bfloat16))

    back2 = f32_dot(jnp.concatenate(hidden, axis=0), wd2).astype(jnp.bfloat16)
    home2 = lax.all_to_all(back2.reshape(n_ep, CAP, flat_width), "ep", 0, 0, tiled=True).reshape(rows, flat_width)

    def down(x, target):
        return f32_dot(x, lax.dynamic_slice_in_dim(wd, target * piece, ring_piece, 1))

    seen = [[[], []], [[], []]]
    for s in range(far, 0, -1):
        for h in range(2):
            for d, perm in enumerate((right, left)):
                if s <= hops[h][d]:
                    target = at(s) if d == 0 else at(-s)
                    so_far = seen[h][d]
                    x = hidden[h]
                    if so_far:
                        tie = max(len(so_far) - 2, 0)
                        x, so_far[tie] = lax.optimization_barrier((x, so_far[tie]))
                    part = down(x, target)
                    if so_far:
                        part = part + so_far[-1].astype(jnp.float32)
                    so_far.append(lax.ppermute(part.astype(jnp.bfloat16), "tp", perm))
    back1 = []
    for h in range(2):
        x, seen[h][0][-2] = lax.optimization_barrier((hidden[h], seen[h][0][-2]))
        total = down(x, me) + seen[h][0][-1].astype(jnp.float32) + seen[h][1][-1].astype(jnp.float32)
        back1.append(total.astype(jnp.bfloat16))
    back1 = jnp.concatenate(back1, axis=0).reshape(n_ep, CAP, ring_piece)
    home1 = lax.all_to_all(back1, "ep", 0, 0, tiled=True).reshape(rows, ring_piece)

    first_dims = (((0,), (0,)), ((), ()))

    def combine(x):
        return f32_dot(weight_high, x, first_dims) + f32_dot(weight_low, x, first_dims)

    mixed2 = combine(home2)
    step = 1
    while step < n_tp:
        size = mixed2.shape[1] // 2
        bit = lax.rem(me // step, 2)
        kept = lax.dynamic_slice_in_dim(mixed2, bit * size, size, 1)
        sent = lax.dynamic_slice_in_dim(mixed2, (1 - bit) * size, size, 1).astype(jnp.bfloat16)
        sent = lax.ppermute(sent, "tp", [(i, i ^ step) for i in range(n_tp)])
        mixed2 = kept + sent.astype(jnp.float32)
        step *= 2
    combined = jnp.concatenate([combine(home1), mixed2], axis=1)

    stats = jnp.stack([jnp.sum(combined, axis=1), jnp.sum(combined * combined, axis=1)])
    stats = lax.all_to_all(jnp.broadcast_to(stats[None], (n_tp, *stats.shape)), "tp", 0, 0, tiled=True)
    stats = jnp.sum(stats, axis=0)
    row_mean = stats[0] / D
    row_var = stats[1] / D - row_mean * row_mean
    normed = (combined - row_mean[:, None]) * lax.rsqrt(
        row_var[:, None] + norm_eps
    ) * norm_gain + norm_bias
    return normed.astype(jnp.bfloat16)


def solution(mesh):
    return jax.shard_map(
        layer,
        mesh=mesh,
        in_specs=(
            P(("grp", "ep"), None),
            P(("grp", "ep"), None),
            P(("grp", "ep"), None),
            P("ep", None, "tp"),
            P("ep", None, "tp"),
            P("ep", "tp", None),
            P("tp"),
            P("tp"),
        ),
        out_specs=P(("grp", "ep"), "tp"),
        check_vma=False,
    )
```
